32 devices in a mesh: sp: 8 (over z, core), tp: 4 (over y, x).
Axes of the slice: x: 2, y: 2, z: 4, core: 2. Of those that a mesh axis runs over, the one named last changes fastest.
Arguments:
- moe_input: bfloat16 [1024, 2048], P('sp', 'tp'), may hold values from -6 to 6
- cotangent: bfloat16 [1024, 2048], P('sp', 'tp'), may hold values from -6 to 6
- routes: int32 [1024, 2], P('sp'), may hold values from 0 to 7, all different within a row; in each aligned block of 128 rows (0 to 127, 128 to 255, ...) at most 40 rows name the same one
- route_weights: float32 [1024, 2], P('sp'), may hold values from 0.2 to 1
- gate_branch: bfloat16 [1024, 2560], P('sp', 'tp'), may hold values from -6 to 6
- log_decay: float32 [1024, 2560], P('sp', 'tp'), may hold values from -0.12 to 0
- states: float32 [1024, 2560], P('sp', 'tp'), may hold values from -6 to 6
- w_gate: bfloat16 [8, 2048, 2048], P('sp', None, 'tp'), may hold values from -0.125 to 0.125
- w_up: bfloat16 [8, 2048, 2048], P('sp', None, 'tp'), may hold values from -0.125 to 0.125
- w_down: bfloat16 [8, 2048, 2048], P('sp', 'tp'), may hold values from -0.125 to 0.125
- out_proj: bfloat16 [2048, 2560], P('sp', 'tp'), may hold values from -0.125 to 0.125
Outputs:
- grad_w_gate: float32 [8, 2048, 2048], P('sp', None, 'tp')
- grad_w_up: float32 [8, 2048, 2048], P('sp', None, 'tp')
- grad_w_down: float32 [8, 2048, 2048], P('sp', 'tp')
- grad_out_proj: float32 [2048, 2560], P('sp', 'tp')
- grad_gate_branch: bfloat16 [1024, 2560], P('sp', 'tp')
- grad_log_decay: bfloat16 [1024, 2560], P('sp', 'tp')
- grad_input_term: float32 [1024, 2560], P('sp', 'tp')
The draws below stay inside these ranges and needn't reach their ends.
Inputs may be any that keep to these rules, and one draw needn't show every extreme that they name: `routes`: in the rows of one device no expert is named by more than 40 entries, and in every draw some expert is named by exactly 40 entries of one device's rows.
All inputs are finite; a program needn't handle non-finite values.
Results may differ from the reference program's by a relative error of at most 0.025.
Values may be sent and summed in bfloat16 or wider, within the bound.
No kernel may reach another device: no remote copies, remote signals or barrier semaphores. Data moves between devices by JAX's collectives and lax.ppermute only.
A program may use at most 64 MiB of HBM per device.

```python
import math
import jax
import jax.numpy as jnp
import numpy as np
from jax import lax

D = 2048
W = 2560
F = 2048
TOP = 2
TOK_DEV = 128
EXPERTS = 8
TOKENS = 1024
CAP = 40
N_SP = 8
N_TP = 4


def draw_log_decay(key, part):
    key_kind, key_rate, key_block, key_cell = jax.random.split(key, 4)
    slow_share = 50
    slow_mask = jax.random.randint(key_kind, (W,), 0, 100) < slow_share
    slow_rate = jax.random.uniform(key_rate, (W,), jnp.float32, 0.3, 0.5) * math.log(10.0) / TOKENS
    fast_rate = jax.random.uniform(jax.random.fold_in(key_rate, 7), (W,), jnp.float32, 1.0 / 60.0, 1.0 / 25.0)
    chan_rates = jnp.where(slow_mask, slow_rate, fast_rate)
    block_scale = jnp.exp(jax.random.uniform(key_block, (TOKENS // TOK_DEV, W), jnp.float32, -math.log(2.0), math.log(2.0)))
    block_scale = jnp.repeat(block_scale, TOK_DEV, axis=0)
    cell_scale = jax.random.uniform(key_cell, (TOKENS, W), jnp.float32, 0.5, 1.5)
    return -(chan_rates[None, :] * block_scale * cell_scale)


def strengthened(entries, rng, source, target, blocks, factor):
    owner, partner = [(jnp.arange(entries.shape[position]) // (entries.shape[position] // blocks)).reshape([-1 if axis == position else 1 for axis in range(entries.ndim)]) for position in (source, target)]
    chosen = jax.random.permutation(rng, blocks)[partner]
    strong = (owner == chosen) | (owner == (partner + blocks // 2) % blocks)
    return jnp.where(strong, factor * entries, entries)


def shard_levels(key, dims, cuts, smallest, largest):
    loudness, own = 1.0, jax.random.fold_in(key, 6)
    for dim, blocks in cuts:
        heights = jnp.exp(jax.random.uniform(jax.random.fold_in(own, dim), (blocks,), jnp.float32, smallest / len(cuts), largest / len(cuts)))
        loudness = loudness * jnp.repeat(heights, dims[dim] // blocks).reshape([-1 if axis == dim else 1 for axis in range(len(dims))])
    return loudness


def deal_out(own_key, own, number, rows, count, top, bound, lean):
    ranking = jax.random.permutation(own_key, count)
    heavy_load, ordinary = load_shares(count, rows * top, bound, lean, True), load_shares(count, rows * top, bound, lean, False)
    places = jnp.arange(count)

    def named(lengths, turn):
        used = int((lengths > 0).sum())
        fixed = max(1, used // 4)
        moved = fixed + (places - fixed + turn * (used - fixed)) % max(1, count - fixed)
        return jnp.zeros((count,), jnp.int32).at[ranking[jnp.where(places < fixed, places, moved)]].set(jnp.asarray(lengths, jnp.int32))

    lengths = jnp.where(number % 4 == 0, named(heavy_load, number // 4), named(ordinary, number - number // 4 - 1))
    mixed = jax.random.permutation(jax.random.fold_in(own, 3), count)
    source_of, taker = mixed[0:count // 2 * 2:2], mixed[1:count // 2 * 2:2]
    slack = jnp.minimum(lengths[source_of] - 1, bound - lengths[taker]) // 2
    slack = jnp.where((source_of == ranking[0]) | (taker == ranking[0]) | (lengths[taker] == 0), 0, jnp.maximum(slack, 0))
    moved = jax.random.randint(jax.random.fold_in(own, 4), (count // 2,), 0, 1 << 20) % (slack + 1)
    lengths = lengths.at[source_of].add(-moved).at[taker].add(moved)
    items = jnp.searchsorted(jnp.cumsum(lengths), jnp.arange(rows * top), side="right").astype(jnp.int32)
    listing = items.reshape(top, rows).T
    listing = listing[jax.random.permutation(jax.random.fold_in(own, 1), rows)]
    turn = jax.random.randint(jax.random.fold_in(own, 2), (rows, 1), 0, top)
    return jnp.take_along_axis(listing, (jnp.arange(top)[None, :] + turn) % top, axis=1)


def load_shares(amount, total, limit, skew, full):
    weights = [(1 << 20) // math.isqrt(standing ** skew) + 1 for standing in range(1, amount + 1)]
    largest = limit if full else min(limit, max(-(-total // amount), total * weights[0] // sum(weights)))
    least = 1 if total - largest >= amount - 1 else 0
    counts, spare = [largest] + [least] * (amount - 1), total - largest - least * (amount - 1)
    while spare > 0:
        free = [i for i in range(1, amount) if counts[i] < largest] or [i for i in range(1, amount) if counts[i] < limit]
        whole, budget = sum([weights[i] for i in free]), spare
        for i in free:
            extra = min(limit - counts[i], max(1, budget * weights[i] // whole), spare)
            counts[i] = counts[i] + extra
            spare = spare - extra
    return np.array(counts)


def gaussian(stream_key, shape, width, bound, cuts=(), kind=jnp.bfloat16):
    result = width * jax.random.normal(stream_key, shape, jnp.float32)
    if cuts:
        result = result * shard_levels(stream_key, shape, cuts, -0.22, 0.18)
    return jnp.clip(result, -bound, bound).astype(kind)


def noise_with(key, shape, deviation, reach, cuts, heavy, kind=jnp.bfloat16):
    result = deviation * jax.random.normal(key, shape, jnp.float32)
    if cuts:
        result = result * shard_levels(key, shape, cuts, -0.22, 0.18)
    return jnp.clip(strengthened(result, jax.random.fold_in(key, 3), *heavy), -reach, reach).astype(kind)


def setup_inputs(seed: int = 0) -> dict:
    key_list = jax.random.split(jax.random.key(seed), 12)
    moe_input = gaussian(key_list[0], (TOKENS, D), 1.0, 6.0, ((0, 8), (1, 4)))
    cotangent = noise_with(key_list[1], (TOKENS, D), 1.0, 6.0, ((0, 8), (1, 4)), (0, 1, 8, 2.0))
    routes_keys = jax.random.split(jax.random.fold_in(key_list[2], 1), TOKENS // TOK_DEV)
    routes_turns = jax.random.permutation(jax.random.fold_in(key_list[2], 3), TOKENS // TOK_DEV)
    routes = jax.vmap(lambda own, number: deal_out(jax.random.fold_in(key_list[2], 2), own, number, TOK_DEV, EXPERTS, TOP, CAP, 2))(routes_keys, routes_turns).reshape((TOKENS, TOP))
    route_weights = jnp.clip(0.2 + 0.8 * jax.random.uniform(key_list[3], (TOKENS, TOP), jnp.float32) ** shard_levels(key_list[3], (TOKENS, TOP), ((0, 8),), -0.2, 0.2), 0.2, 1.0)
    gate_branch = gaussian(key_list[4], (TOKENS, W), 1.0, 6.0, ((0, 8), (1, 4)))
    log_decay = draw_log_decay(jax.random.fold_in(key_list[11], 71), 0)
    states = gaussian(key_list[6], (TOKENS, W), 1.0, 6.0, ((0, 8), (1, 4)), jnp.float32)
    w_gate = gaussian(key_list[7], (EXPERTS, D, F), D ** -0.5, 0.125, ((0, 8), (2, 4)))
    w_up = gaussian(key_list[8], (EXPERTS, D, F), D ** -0.5, 0.125, ((0, 8), (2, 4)))
    w_down = gaussian(key_list[9], (EXPERTS, F, D), F ** -0.5, 0.125, ((0, 8), (1, 4)))
    out_proj = gaussian(key_list[10], (D, W), W ** -0.5, 0.125, ((0, 8), (1, 4)))
    return dict(moe_input=moe_input, cotangent=cotangent, routes=routes, route_weights=route_weights, gate_branch=gate_branch, log_decay=log_decay, states=states, w_gate=w_gate, w_up=w_up, w_down=w_down, out_proj=out_proj)


def silu_parts(pre_gate):
    sigmoid_val = jax.nn.sigmoid(pre_gate)
    return (pre_gate * sigmoid_val, sigmoid_val * (1.0 + pre_gate * (1.0 - sigmoid_val)))

def combine_pair(left_pair, right_pair):
    return (left_pair[0] * right_pair[0], right_pair[0] * left_pair[1] + right_pair[1])

def expert_backward(row_data, scaled, gate_w, up_w, down_w):
    pre_gate = jnp.dot(row_data, gate_w, preferred_element_type=jnp.float32)
    pre_up = jnp.dot(row_data, up_w, preferred_element_type=jnp.float32)
    active, slope = silu_parts(pre_gate)
    hidden = (active * pre_up).astype(jnp.bfloat16)
    grad_down = jnp.dot(hidden.T, scaled, preferred_element_type=jnp.float32)
    grad_hidden = jnp.dot(scaled, down_w.T, preferred_element_type=jnp.float32)
    grad_pre_gate = (grad_hidden * pre_up * slope).astype(jnp.bfloat16)
    grad_pre_up = (grad_hidden * active).astype(jnp.bfloat16)
    grad_gate_w = jnp.dot(row_data.T, grad_pre_gate, preferred_element_type=jnp.float32)
    grad_up_w = jnp.dot(row_data.T, grad_pre_up, preferred_element_type=jnp.float32)
    row_total = grad_pre_gate.shape[0]
    blocked_gate = grad_pre_gate.reshape(row_total, N_TP, F // N_TP).astype(jnp.float32)
    blocked_up = grad_pre_up.reshape(row_total, N_TP, F // N_TP).astype(jnp.float32)
    weight_gate = gate_w.reshape(D, N_TP, F // N_TP).astype(jnp.float32)
    weight_up = up_w.reshape(D, N_TP, F // N_TP).astype(jnp.float32)
    block_terms = jnp.einsum('nbf,dbf->bnd', blocked_gate, weight_gate) + jnp.einsum('nbf,dbf->bnd', blocked_up, weight_up)
    rounded = lax.optimization_barrier(block_terms.astype(jnp.bfloat16))
    entry_grad = lax.optimization_barrier(jnp.sum(rounded.astype(jnp.float32), axis=0)).astype(jnp.bfloat16)
    return (grad_gate_w, grad_up_w, grad_down, entry_grad)

def reference(moe_input, cotangent, routes, route_weights, gate_branch, log_decay, states, w_gate, w_up, w_down, out_proj):
    flat_routes = routes.reshape(-1).astype(jnp.int32)
    flat_weights = route_weights.reshape(-1)
    owners = jnp.arange(TOKENS * TOP, dtype=jnp.int32) // TOP
    room = N_SP * CAP

    def per_expert(totals, inputs):
        expert, gate_w, up_w, down_w = inputs
        sorted_idx = jnp.argsort((flat_routes != expert).astype(jnp.int32), stable=True)[:room].astype(jnp.int32)
        live_rows = (flat_routes[sorted_idx] == expert).astype(jnp.float32)
        token_idx = owners[sorted_idx]
        row_data = moe_input[token_idx]
        scaled = ((live_rows * flat_weights[sorted_idx])[:, None] * cotangent[token_idx].astype(jnp.float32)).astype(jnp.bfloat16)
        grad_gate_w, grad_up_w, grad_down, entry_grad = expert_backward(row_data, scaled, gate_w, up_w, down_w)
        totals = totals.at[token_idx].add(entry_grad.astype(jnp.float32) * live_rows[:, None])
        return (totals, (grad_gate_w, grad_up_w, grad_down))
    totals, grads = lax.scan(per_expert, jnp.zeros((TOKENS, D), jnp.float32), (jnp.arange(EXPERTS, dtype=jnp.int32), w_gate, w_up, w_down))
    grad_w_gate, grad_w_up, grad_w_down = grads
    grad_tokens = (cotangent.astype(jnp.float32) + totals).astype(jnp.bfloat16)
    active_gate, pullback = jax.vjp(jax.nn.gelu, gate_branch.astype(jnp.float32))
    mixed_in = (active_gate * states).astype(jnp.bfloat16)
    grad_out_proj = jnp.dot(grad_tokens.T, mixed_in, preferred_element_type=jnp.float32)
    grad_mixed = jnp.dot(grad_tokens, out_proj, preferred_element_type=jnp.float32)
    grad_gate_branch = pullback(grad_mixed * states)[0].astype(jnp.bfloat16)
    grad_state = grad_mixed * active_gate
    decays = jnp.exp(log_decay)
    next_decay = jnp.concatenate([decays[1:], jnp.zeros_like(decays[:1])], axis=0)
    _, back_flip = lax.associative_scan(combine_pair, (jnp.flip(next_decay, 0), jnp.flip(grad_state, 0)))
    grad_input_term = jnp.flip(back_flip, 0)
    prev_states = jnp.concatenate([jnp.zeros_like(states[:1]), states[:-1]], axis=0)
    grad_log_decay = (grad_input_term * decays * prev_states).astype(jnp.bfloat16)
    return (grad_w_gate, grad_w_up, grad_w_down, grad_out_proj, grad_gate_branch, grad_log_decay, grad_input_term)
```

```python
import functools

import jax
import jax.numpy as jnp
from jax import lax
from jax.experimental import pallas as pl
from jax.experimental.pallas import tpu as pltpu
from jax.sharding import PartitionSpec as P


F32 = jnp.float32
BF16 = jnp.bfloat16


def contract_rows(left_mat, right_mat):
    return lax.dot_general(
        left_mat, right_mat, (((0,), (0,)), ((), ())), preferred_element_type=F32
    )


def contract_cols(left_mat, right_mat):
    return lax.dot_general(
        left_mat, right_mat, (((1,), (1,)), ((), ())), preferred_element_type=F32
    )


def swap(value, axis, bits):
    count = lax.axis_size(axis)
    return lax.ppermute(value, axis, [(i, i ^ bits) for i in range(count)])


def vmem_specs(count):
    return [pl.BlockSpec(memory_space=pltpu.VMEM)] * count


def room_for(mebibytes):
    return pltpu.CompilerParams(vmem_limit_bytes=mebibytes * 1024 * 1024)


def kept(value):
    return pltpu.with_memory_space_constraint(value, pltpu.VMEM)


def kept_all(values):
    return [kept(value) for value in values]


def slots_body(groups, room, me_ref, routes_ref, weights_ref, x_ref, c_ref, *outs):
    picks, rows = routes_ref.shape
    chips = groups // 2
    relative = routes_ref[...] ^ me_ref[0]
    expert = lax.broadcasted_iota(jnp.int32, (groups, rows), 0)
    hits = [expert == relative[k : k + 1] for k in range(picks)]
    total = sum(hit.astype(F32) for hit in hits)
    earlier = lax.broadcasted_iota(jnp.int32, (rows, rows), 0) < lax.broadcasted_iota(
        jnp.int32, (rows, rows), 1
    )
    before = jnp.dot(
        total.astype(BF16), earlier.astype(F32).astype(BF16), preferred_element_type=F32
    )
    place = (expert * room).astype(F32) + before
    slot = lax.broadcasted_iota(jnp.int32, (groups * room, rows), 0)
    taken = jnp.zeros((groups * room, rows), F32)
    weight = jnp.zeros((groups * room, rows), F32)
    for k in range(picks):
        target = jnp.sum(jnp.where(hits[k], place, 0.0), axis=0, keepdims=True)
        here = slot == target.astype(jnp.int32)
        taken = jnp.where(here, 1.0, taken)
        weight = jnp.where(here, weights_ref[k : k + 1], weight)
    chosen = taken.astype(BF16)
    slot_weight = jnp.sum(weight, axis=1, keepdims=True)
    data = jnp.dot(chosen, x_ref[...], preferred_element_type=F32).astype(BF16)
    cot = (slot_weight * jnp.dot(chosen, c_ref[...], preferred_element_type=F32)).astype(BF16)
    for k in range(chips):
        outs[k][...] = data[2 * k * room : 2 * (k + 1) * room]
        outs[chips + k][...] = cot[2 * k * room : 2 * (k + 1) * room]
    outs[2 * chips][...] = chosen


def slots(me, routes, weights, x, c, groups, room):
    rows, width = x.shape
    chips = groups // 2
    piece = pltpu.VMEM((2 * room, width), BF16)
    out = pl.pallas_call(
        functools.partial(slots_body, groups, room),
        out_shape=[piece] * (2 * chips) + [pltpu.VMEM((groups * room, rows), BF16)],
        in_specs=[pl.BlockSpec(memory_space=pltpu.SMEM)] + vmem_specs(4),
        out_specs=vmem_specs(2 * chips + 1),
        compiler_params=room_for(8),
        name="slots",
    )(me, *[pltpu.with_memory_space_constraint(v, pltpu.HBM) for v in (routes, weights, x, c)])
    return out[:chips], out[chips : 2 * chips], out[2 * chips]


def forward_body(parts, order_ref, *refs):
    xs, (gate_w, up_w, pre_gate, pre_up) = refs[:parts], refs[parts:]
    width = xs[0].shape[1]
    for k in range(parts):
        at = pl.ds(pl.multiple_of(order_ref[k] * width, width), width)
        x = xs[k][...]
        gate = jnp.dot(x, gate_w[0, at, :], preferred_element_type=F32)
        up = jnp.dot(x, up_w[0, at, :], preferred_element_type=F32)
        if k == 0:
            pre_gate[...] = gate
            pre_up[...] = up
        else:
            pre_gate[...] += gate
            pre_up[...] += up


def forward(order, xs, w_gate, w_up):
    parts = len(xs)
    rows = xs[0].shape[0]
    hid = w_gate.shape[2]
    return pl.pallas_call(
        functools.partial(forward_body, parts),
        out_shape=[pltpu.VMEM((rows, hid), F32)] * 2,
        in_specs=[pl.BlockSpec(memory_space=pltpu.SMEM)] + vmem_specs(parts + 2),
        out_specs=vmem_specs(2),
        compiler_params=room_for(6),
        name="expert_forward",
    )(order, *kept_all([*xs, w_gate, w_up]))


def backward_body(parts, order_ref, *refs):
    cs, refs = refs[:parts], refs[parts:]
    down_w, gate_w, up_w, pre_gate, pre_up, hidden, grad_gate, grad_up = refs[:8]
    terms, total = refs[8 : 8 + parts], refs[8 + parts]
    width = cs[0].shape[1]
    spots = [pl.ds(pl.multiple_of(order_ref[k] * width, width), width) for k in range(parts)]
    for k in range(parts):
        part = contract_cols(cs[k][...], down_w[0, :, spots[k]])
        if k == 0:
            total[...] = part
        else:
            total[...] += part
    grad_hidden = total[...]
    gate, up = pre_gate[...], pre_up[...]
    sig = jax.nn.sigmoid(gate)
    active = gate * sig
    slope = sig * (1.0 + gate * (1.0 - sig))
    hidden[...] = (active * up).astype(BF16)
    grad_gate[...] = (grad_hidden * up * slope).astype(BF16)
    grad_up[...] = (grad_hidden * active).astype(BF16)
    for k in range(parts):
        term = contract_cols(grad_gate[...], gate_w[0, spots[k], :])
        term += contract_cols(grad_up[...], up_w[0, spots[k], :])
        terms[k][...] = term.astype(BF16)


def backward(order, cs, w_down, w_gate, w_up, pre_gate, pre_up):
    parts = len(cs)
    rows, width = cs[0].shape
    hid = w_gate.shape[2]
    out = pl.pallas_call(
        functools.partial(backward_body, parts),
        out_shape=[pltpu.VMEM((rows, hid), BF16)] * 3 + [pltpu.VMEM((rows, width), BF16)] * parts,
        in_specs=[pl.BlockSpec(memory_space=pltpu.SMEM)] + vmem_specs(parts + 5),
        out_specs=vmem_specs(3 + parts),
        scratch_shapes=[pltpu.VMEM((rows, hid), F32)],
        compiler_params=room_for(8),
        name="expert_backward",
    )(order, *kept_all([*cs, w_down, w_gate, w_up, pre_gate, pre_up]))
    return out[0], out[1], out[2], out[3:]


def weights_body(parts, order_ref, *refs):
    xs, cs, refs = refs[:parts], refs[parts : 2 * parts], refs[2 * parts :]
    hidden, grad_gate, grad_up, out_gate, out_up, out_down = refs
    step = pl.program_id(0)
    for k in range(parts):

        @pl.when(step == k)
        def _():
            x = xs[k][...]
            out_gate[0] = contract_rows(x, grad_gate[...])
            out_up[0] = contract_rows(x, grad_up[...])
            out_down[0] = contract_rows(hidden[...], cs[k][...])


def weight_grads(order, xs, cs, hidden, grad_gate, grad_up):
    parts = len(xs)
    _, width = xs[0].shape
    hid = hidden.shape[1]
    model = width * parts
    wide = pl.BlockSpec((1, width, hid), lambda i, o: (0, o[i], 0))
    down = pl.BlockSpec((1, hid, width), lambda i, o: (0, 0, o[i]))
    return pl.pallas_call(
        functools.partial(weights_body, parts),
        out_shape=[jax.ShapeDtypeStruct((1, model, hid), F32)] * 2
        + [jax.ShapeDtypeStruct((1, hid, model), F32)],
        grid_spec=pltpu.PrefetchScalarGridSpec(
            num_scalar_prefetch=1,
            grid=(parts,),
            in_specs=vmem_specs(2 * parts + 3),
            out_specs=[wide, wide, down],
        ),
        compiler_params=room_for(14),
        name="weight_grads",
    )(order, *kept_all([*xs, *cs, hidden, grad_gate, grad_up]))


def combine_body(count, chosen_ref, cot_ref, *refs):
    backs, out = refs[:count], refs[count]
    piece = backs[0].shape[0]
    total = cot_ref[...].astype(F32)
    for k in range(count):
        total += contract_rows(chosen_ref[k * piece : (k + 1) * piece], backs[k][...])
    out[...] = total.astype(BF16)


def combine(chosen, cot, backs):
    return pl.pallas_call(
        functools.partial(combine_body, len(backs)),
        out_shape=pltpu.VMEM(cot.shape, BF16),
        in_specs=vmem_specs(2 + len(backs)),
        out_specs=vmem_specs(1)[0],
        compiler_params=room_for(6),
        name="combine",
    )(*kept_all([chosen, cot, *backs]))


def gates_body(gate_ref, states_ref, active_ref, pull_ref, mixed_ref):
    gate = gate_ref[...].astype(F32)
    states = states_ref[...]
    coef = 0.7978845608028654
    inner = jnp.tanh(coef * (gate + 0.044715 * gate * gate * gate))
    half = 0.5 * (1.0 + inner)
    active = gate * half
    slope = half + 0.5 * gate * (1.0 - inner * inner) * coef * (
        1.0 + 3.0 * 0.044715 * gate * gate
    )
    active_ref[...] = active
    pull_ref[...] = states * slope
    mixed_ref[...] = (active * states).astype(BF16)


def gates(gate_branch, states):
    full = jax.ShapeDtypeStruct(states.shape, F32)
    return pl.pallas_call(
        gates_body,
        out_shape=[full, full, pltpu.VMEM(states.shape, BF16)],
        in_specs=vmem_specs(2),
        out_specs=vmem_specs(3),
        compiler_params=room_for(8),
        name="gates",
    )(gate_branch, states)


def recur_body(me_ref, tokens_ref, own_ref, other_ref, active_ref, pull_ref, log_ref,
               gate_out, local_out, span_out, edge_out):
    chips, rows, width = tokens_ref.shape
    half = width // 2
    first = (me_ref[0] & 1) == 0
    chip = me_ref[0] // 2
    mixed = jnp.zeros((rows, own_ref.shape[2]), F32)
    for k in range(chips):
        block = tokens_ref[chip ^ k]
        left, right = block[:, :half], block[:, half:]
        mine = jnp.where(first, left, right)
        theirs = jnp.where(first, right, left)
        mixed += jnp.dot(mine, own_ref[k, :half], preferred_element_type=F32)
        mixed += jnp.dot(theirs, other_ref[k, :half], preferred_element_type=F32)
    gate_out[...] = (mixed * pull_ref[...]).astype(BF16)
    value = mixed * active_ref[...]
    decays = jnp.exp(log_ref[...])
    row = lax.broadcasted_iota(jnp.int32, decays.shape, 0)
    factor = jnp.where(row == rows - 1, 1.0, pltpu.roll(decays, rows - 1, 0))
    inside = row % 8
    for step in (1, 2, 4):
        keep = inside + step < 8
        value_next = pltpu.roll(value, rows - step, 0)
        factor_next = pltpu.roll(factor, rows - step, 0)
        value = value + jnp.where(keep, factor * value_next, 0.0)
        factor = jnp.where(keep, factor * factor_next, factor)
    carry = jnp.zeros((1, decays.shape[1]), F32)
    span = jnp.ones((1, decays.shape[1]), F32)
    for block in range(rows // 8 - 1, -1, -1):
        at = slice(block * 8, block * 8 + 8)
        local = value[at] + factor[at] * carry
        spans = factor[at] * span
        local_out[at] = local
        span_out[at] = spans
        carry, span = local[:1], spans[:1]
    lead = decays[:1]
    edge_row = lax.broadcasted_iota(jnp.int32, edge_out.shape, 0)
    edge_out[...] = jnp.where(edge_row == 0, lead * span, lead * carry)


def recur(me, tokens, own, other, active, pull, log_decay):
    full = pltpu.VMEM(log_decay.shape, F32)
    return pl.pallas_call(
        recur_body,
        out_shape=[
            jax.ShapeDtypeStruct(log_decay.shape, BF16),
            full,
            full,
            pltpu.VMEM((8, log_decay.shape[1]), F32),
        ],
        in_specs=[pl.BlockSpec(memory_space=pltpu.SMEM)] + vmem_specs(6),
        out_specs=vmem_specs(4),
        compiler_params=room_for(8),
        name="recur",
    )(me, *kept_all([tokens, own, other, active, pull, log_decay]))


def finish_body(me_ref, own_ref, other_ref, local_ref, span_ref, past_ref, term_out, log_out):
    count = 2 * own_ref.shape[0]
    me = me_ref[0]

    def turn(i, carry):
        place = count - 1 - i
        relative = place ^ me
        mine, theirs = own_ref[relative // 2], other_ref[relative // 2]
        edge = jnp.where((relative & 1) == 0, mine, theirs)
        return jnp.where(place > me, edge[1:2] + edge[:1] * carry, carry)

    carry = lax.fori_loop(0, count - 1, turn, jnp.zeros((1, local_ref.shape[1]), F32))
    term = local_ref[...] + span_ref[...] * carry
    term_out[...] = term
    log_out[...] = (term * past_ref[...]).astype(BF16)


def finish(me, own, other, local, span, past):
    return pl.pallas_call(
        finish_body,
        out_shape=[
            jax.ShapeDtypeStruct(local.shape, F32),
            jax.ShapeDtypeStruct(local.shape, BF16),
        ],
        in_specs=[pl.BlockSpec(memory_space=pltpu.SMEM)] + vmem_specs(5),
        out_specs=vmem_specs(2),
        compiler_params=room_for(6),
        name="finish",
    )(me, *kept_all([own, other, local, span, past]))


def spread_body(me_ref, tokens_ref, *outs):
    for k, out in enumerate(outs):
        out[...] = tokens_ref[(me_ref[0] // 2) ^ k]


def spread(me, tokens):
    chips, rows, width = tokens.shape
    return pl.pallas_call(
        spread_body,
        out_shape=[pltpu.VMEM((rows, width), BF16)] * chips,
        in_specs=[pl.BlockSpec(memory_space=pltpu.SMEM)] + vmem_specs(1),
        out_specs=vmem_specs(chips),
        compiler_params=room_for(4),
        name="spread",
    )(me, kept(tokens))


def halves_body(me_ref, *refs):
    got, (own, other) = refs[:-2], refs[-2:]
    first = (me_ref[0] & 1) == 0
    half = own.shape[2]
    for k, piece in enumerate(got):
        left, right = piece[:, :half], piece[:, half:]
        own[k] = jnp.where(first, left, right)
        other[k] = jnp.where(first, right, left)


def halves(me, got):
    rows, width = got[0].shape
    return pl.pallas_call(
        halves_body,
        out_shape=[pltpu.VMEM((len(got), rows, width // 2), BF16)] * 2,
        in_specs=[pl.BlockSpec(memory_space=pltpu.SMEM)] + vmem_specs(len(got)),
        out_specs=vmem_specs(2),
        compiler_params=room_for(4),
        name="halves",
    )(me, *kept_all(got))


def proj_body(tok_own, tok_other, own_ref, other_ref, out):
    chips, rows, _ = tok_own.shape
    skip = own_ref.shape[1] - rows
    total = jnp.zeros(out.shape, F32)
    for k in range(chips):
        total += contract_rows(tok_own[k], own_ref[k, skip:])
    for k in range(chips):
        total += contract_rows(tok_other[k], other_ref[k, skip:])
    out[...] = total


def proj_grad(tok_own, tok_other, own, other):
    return pl.pallas_call(
        proj_body,
        out_shape=jax.ShapeDtypeStruct((tok_own.shape[2], own.shape[2]), F32),
        in_specs=vmem_specs(4),
        out_specs=vmem_specs(1)[0],
        compiler_params=room_for(6),
        name="proj_grad",
    )(*kept_all([tok_own, tok_other, own, other]))


def shards(
    moe_input,
    cotangent,
    routes,
    route_weights,
    gate_branch,
    log_decay,
    states,
    w_gate,
    w_up,
    w_down,
    out_proj,
):
    groups = lax.axis_size("sp")
    parts = lax.axis_size("tp")
    chips = groups // 2
    tok_rows, picks = routes.shape
    room = tok_rows * picks * 5 // (4 * groups)
    me = lax.axis_index("sp").astype(jnp.int32).reshape(1)
    order = lax.axis_index("tp").astype(jnp.int32) ^ jnp.arange(parts, dtype=jnp.int32)

    send_x, send_c, chosen = slots(
        me, routes.T, route_weights.T, moe_input, cotangent, groups, room
    )

    def between_chips(pieces):
        return [pieces[0]] + [swap(pieces[k], "sp", 2 * k) for k in range(1, chips)]

    def between_cores(got):
        other = swap(jnp.concatenate([piece[room:] for piece in got], axis=0), "sp", 1)
        return jnp.concatenate([piece[:room] for piece in got] + [other], axis=0)

    def between_parts(pieces):
        return [pieces[0]] + [swap(pieces[k], "tp", k) for k in range(1, parts)]

    got_x, got_c = between_chips(send_x), between_chips(send_c)
    earlier_state = lax.ppermute(
        states[-1:], "sp", [(source, source + 1) for source in range(groups - 1)]
    )
    past = jnp.exp(log_decay) * jnp.concatenate([earlier_state, states[:-1]], axis=0)
    active, pull, mixed_in = gates(gate_branch, states)
    bundle = jnp.concatenate([out_proj, mixed_in], axis=0)
    xs = between_parts([between_cores(got_x)] * parts)
    cs = between_parts([between_cores(got_c)] * parts)
    bundles = jnp.stack(between_chips([bundle] * chips))
    bundles_other = swap(bundles, "sp", 1)

    pre_gate, pre_up = forward(order, xs, w_gate, w_up)
    hidden, grad_gate, grad_up, terms = backward(
        order, cs, w_down, w_gate, w_up, pre_gate, pre_up
    )
    shares = between_parts(terms)
    grad_gate_w, grad_up_w, grad_down = weight_grads(
        order, xs, cs, hidden, grad_gate, grad_up
    )
    summed = sum(share.astype(F32) for share in shares).astype(BF16)

    near, far = summed[: chips * room], swap(summed[chips * room :], "sp", 1)
    spans = [slice(k * room, (k + 1) * room) for k in range(chips)]
    backs = [jnp.concatenate([near[at], far[at]], axis=0) for at in spans]
    backs = between_chips(backs)
    grad_cols = combine(chosen, cotangent, backs)
    tokens = lax.all_gather(grad_cols, "tp", axis=0)
    if parts != chips:
        model = parts * grad_cols.shape[1]
        tokens = tokens.transpose(1, 0, 2).reshape(tok_rows, chips, model // chips)
        tokens = tokens.transpose(1, 0, 2)

    got = between_chips(spread(me, tokens))
    grad_gate_branch, local, span, edge = recur(
        me, tokens, bundles, bundles_other, active, pull, log_decay
    )
    edges = jnp.stack(between_chips([edge] * chips))
    edges_other = swap(edges, "sp", 1)
    tok_own, tok_other = halves(me, got)
    tok_other = swap(tok_other, "sp", 1)
    grad_input_term, grad_log_decay = finish(me, edges, edges_other, local, span, past)
    grad_out_proj = proj_grad(tok_own, tok_other, bundles, bundles_other)
    return (
        grad_gate_w,
        grad_up_w,
        grad_down,
        grad_out_proj,
        grad_gate_branch,
        grad_log_decay,
        grad_input_term,
    )


def solution(mesh):
    return jax.shard_map(
        shards,
        mesh=mesh,
        in_specs=(
            P("sp", "tp"),
            P("sp", "tp"),
            P("sp", None),
            P("sp", None),
            P("sp", "tp"),
            P("sp", "tp"),
            P("sp", "tp"),
            P("sp", None, "tp"),
            P("sp", None, "tp"),
            P("sp", "tp", None),
            P("sp", "tp"),
        ),
        out_specs=(
            P("sp", None, "tp"),
            P("sp", None, "tp"),
            P("sp", "tp", None),
            P("sp", "tp"),
            P("sp", "tp"),
            P("sp", "tp"),
            P("sp", "tp"),
        ),
        check_vma=False,
    )
```
